256 devices in a mesh: sp: 64 (over z, y, core), tp: 4 (over x).
Axes of the slice: x: 4, y: 4, z: 8, core: 2. Of those that a mesh axis runs over, the one named last changes fastest.
Arguments:
- b_gate: bfloat16 [32768, 2048], P('sp', 'tp'), may hold values from -6 to 6
- c_gate: bfloat16 [32768, 2048], P('sp', 'tp'), may hold values from -6 to 6
- values_in: bfloat16 [32768, 2048], P('sp', 'tp'), may hold values from -6 to 6
- conv_taps: float32 [3, 2048], P(None, 'tp'), may hold values from -4 to 4
- out_proj: bfloat16 [2048, 2048], P('tp'), may hold values from -0.125 to 0.125
- resid: bfloat16 [32768, 2048], P(('sp', 'tp')), may hold values from -6 to 6
- post_gain: float32 [2048], replicated, may hold values from 0.1 to 1.9
- pre_gain: float32 [2048], replicated, may hold values from 0.1 to 1.9
- moe_gain: float32 [2048], replicated, may hold values from 0.1 to 1.9
- routes: int32 [32768, 4], P(('sp', 'tp')), may hold values from 0 to 63, all different within a row; in each aligned block of 128 rows (0 to 127, 128 to 255, ...) at most 16 rows name the same one
- route_weight: float32 [32768, 4], P(('sp', 'tp')), may hold values from 0.1 to 1
- gate_w: bfloat16 [64, 2048, 640], P('sp'), may hold values from -1 to 1
- up_w: bfloat16 [64, 2048, 640], P('sp'), may hold values from -1 to 1
- down_w: bfloat16 [64, 640, 2048], P('sp'), may hold values from -0.25 to 0.25
Outputs:
- result: bfloat16 [32768, 2048], P(('sp', 'tp'))
The draws below stay inside these ranges and needn't reach their ends.
Inputs may be any that keep to these rules, and one draw needn't show every extreme that they name: `routes`: each row names 4 different experts; within each aligned block of 128 rows no expert is named by more than 16 rows.
All inputs are finite; a program needn't handle non-finite values.
Results may differ from the reference program's by a relative error of at most 0.007.
Values may be sent and summed in bfloat16 or wider, within the bound.
A program may use at most 64 MiB of HBM per device.

```python
import math
import jax
import jax.numpy as jnp
import numpy as np
from jax import lax

D = 2048
FF = 640
TOPK = 4
ROWS = 128
TOKENS = 32768
EXPERTS = 64
CAP = 16
N_SP = 64
N_TP = 4


def expert_matrix(key):
    scale = D ** (-0.5)
    sample = jax.random.normal(key, (EXPERTS, D, FF), jnp.float32) * scale
    return jnp.clip(sample, -1.0, 1.0).astype(jnp.bfloat16)


def draw_gate_w(key, part):
    return expert_matrix(jax.random.fold_in(key, 11))


def draw_up_w(key, part):
    return expert_matrix(jax.random.fold_in(key, 23))


def steps_of(stream_key, extent, pieces, low, largest):
    level, own = 1.0, jax.random.fold_in(stream_key, 6)
    for position, blocks in pieces:
        heights = jnp.exp(jax.random.uniform(jax.random.fold_in(own, position), (blocks,), jnp.float32, low / len(pieces), largest / len(pieces)))
        level = level * jnp.repeat(heights, extent[position] // blocks).reshape([-1 if axis == position else 1 for axis in range(len(extent))])
    return level


def deal_out(stream_key, own, number, rows, number_of, top, most, lean):
    ranking = jax.random.permutation(stream_key, number_of)
    crowded, ordinary = shares(number_of, rows * top, most, lean, True), shares(number_of, rows * top, most, lean, False)
    places = jnp.arange(number_of)

    def named(lengths, offset_by):
        used = int((lengths > 0).sum())
        fixed = max(1, used // 4)
        passed = fixed + (places - fixed + offset_by * (used - fixed)) % max(1, number_of - fixed)
        return jnp.zeros((number_of,), jnp.int32).at[ranking[jnp.where(places < fixed, places, passed)]].set(jnp.asarray(lengths, jnp.int32))

    lengths = jnp.where(number % 4 == 0, named(crowded, number // 4), named(ordinary, number - number // 4 - 1))
    mixed = jax.random.permutation(jax.random.fold_in(own, 3), number_of)
    source_of, sink = mixed[0:number_of // 2 * 2:2], mixed[1:number_of // 2 * 2:2]
    margin = jnp.minimum(lengths[source_of] - 1, most - lengths[sink]) // 2
    margin = jnp.where((source_of == ranking[0]) | (sink == ranking[0]) | (lengths[sink] == 0), 0, jnp.maximum(margin, 0))
    passed = jax.random.randint(jax.random.fold_in(own, 4), (number_of // 2,), 0, 1 << 20) % (margin + 1)
    lengths = lengths.at[source_of].add(-passed).at[sink].add(passed)
    labels = jnp.searchsorted(jnp.cumsum(lengths), jnp.arange(rows * top), side="right").astype(jnp.int32)
    listing = labels.reshape(top, rows).T
    listing = listing[jax.random.permutation(jax.random.fold_in(own, 1), rows)]
    offset_by = jax.random.randint(jax.random.fold_in(own, 2), (rows, 1), 0, top)
    return jnp.take_along_axis(listing, (jnp.arange(top)[None, :] + offset_by) % top, axis=1)


def shares(amount, total, most, skew, full):
    portions = [(1 << 20) // math.isqrt(standing ** skew) + 1 for standing in range(1, amount + 1)]
    largest = most if full else min(most, max(-(-total // amount), total * portions[0] // sum(portions)))
    least = 1 if total - largest >= amount - 1 else 0
    holding, surplus = [largest] + [least] * (amount - 1), total - largest - least * (amount - 1)
    while surplus > 0:
        free = [i for i in range(1, amount) if holding[i] < largest] or [i for i in range(1, amount) if holding[i] < most]
        mass, budget = sum([portions[i] for i in free]), surplus
        for i in free:
            more = min(most - holding[i], max(1, budget * portions[i] // mass), surplus)
            holding[i] = holding[i] + more
            surplus = surplus - more
    return np.array(holding)


def bell_draw(key, extent, width, most, cuts=(), kind=jnp.bfloat16):
    drawn = jax.random.normal(key, extent, jnp.float32) * width
    if len(cuts) > 0:
        drawn = steps_of(key, extent, cuts, -0.22, 0.18) * drawn
    return jnp.clip(drawn, min=-most, max=most).astype(kind)


def setup_inputs(seed: int = 0) -> dict:
    arg_keys = jax.random.split(jax.random.key(seed), 15)
    b_gate = bell_draw(arg_keys[0], (TOKENS, D), 1.0, 6.0, ((0, 64), (1, 4)))
    c_gate = bell_draw(arg_keys[1], (TOKENS, D), 1.0, 6.0, ((0, 64), (1, 4)))
    values_in = bell_draw(arg_keys[2], (TOKENS, D), 1.0, 6.0, ((0, 64), (1, 4)))
    conv_taps = bell_draw(arg_keys[3], (3, D), 0.577, 4.0, ((1, 4),), jnp.float32)
    out_proj = bell_draw(arg_keys[4], (D, D), D ** -0.5, 0.125, ((0, 4),))
    resid = bell_draw(arg_keys[5], (TOKENS, D), 1.0, 6.0, ((0, 256),))
    post_gain = jnp.clip(1.0 + 0.18 * jax.random.normal(arg_keys[6], (D,), jnp.float32), 0.1, 1.9)
    pre_gain = jnp.clip(1.0 + 0.18 * jax.random.normal(arg_keys[7], (D,), jnp.float32), 0.1, 1.9)
    moe_gain = jnp.clip(1.0 + 0.18 * jax.random.normal(arg_keys[8], (D,), jnp.float32), 0.1, 1.9)
    routes_keys = jax.random.split(jax.random.fold_in(arg_keys[9], 1), TOKENS // ROWS)
    routes_turns = jax.random.permutation(jax.random.fold_in(arg_keys[9], 3), TOKENS // ROWS)
    routes = jax.vmap(lambda own, number: deal_out(jax.random.fold_in(arg_keys[9], 2), own, number, ROWS, EXPERTS, TOPK, CAP, 1))(routes_keys, routes_turns).reshape((TOKENS, TOPK))
    route_weight = jnp.clip(0.1 + 0.9 * jax.random.uniform(arg_keys[10], (TOKENS, TOPK), jnp.float32) ** steps_of(arg_keys[10], (TOKENS, TOPK), ((0, 256),), -0.2, 0.2), 0.1, 1.0)
    gate_w = draw_gate_w(jax.random.fold_in(arg_keys[14], 71), 0)
    up_w = draw_up_w(jax.random.fold_in(arg_keys[14], 71), 0)
    down_w = bell_draw(arg_keys[13], (EXPERTS, FF, D), FF ** -0.5, 0.25, ((0, 64),))
    return {"b_gate": b_gate, "c_gate": c_gate, "values_in": values_in, "conv_taps": conv_taps, "out_proj": out_proj, "resid": resid, "post_gain": post_gain, "pre_gain": pre_gain, "moe_gain": moe_gain, "routes": routes, "route_weight": route_weight, "gate_w": gate_w, "up_w": up_w, "down_w": down_w}


epsilon = 1e-06

def rms_norm(vector, gain):
    return vector * lax.rsqrt(lax.optimization_barrier(jnp.mean(vector * vector, axis=-1, keepdims=True)) + epsilon) * gain

def reference(b_gate, c_gate, values_in, conv_taps, out_proj, resid, post_gain, pre_gain, moe_gain, routes, route_weight, gate_w, up_w, down_w):
    length = b_gate.shape[0]
    product = c_gate.astype(jnp.float32) * values_in.astype(jnp.float32)
    padded = jnp.pad(product, ((2, 0), (0, 0)))
    filtered = padded[0:length] * conv_taps[0] + padded[1:length + 1] * conv_taps[1] + padded[2:length + 2] * conv_taps[2]
    mixed = (b_gate.astype(jnp.float32) * filtered).astype(jnp.bfloat16)
    projected = jnp.dot(mixed, out_proj, preferred_element_type=jnp.float32)
    stream = (resid.astype(jnp.float32) + rms_norm(projected, post_gain)).astype(jnp.bfloat16)
    normed = rms_norm(stream.astype(jnp.float32), pre_gain).astype(jnp.bfloat16)
    flat_ids = routes.reshape(-1).astype(jnp.int32)
    flat_weight = route_weight.reshape(-1)
    assigned = flat_ids.shape[0]
    order = jnp.argsort(flat_ids, stable=True).astype(jnp.int32)
    counts = jnp.bincount(flat_ids, length=EXPERTS).astype(jnp.int32)
    starts = (jnp.cumsum(counts) - counts).astype(jnp.int32)
    bound = CAP * N_SP * N_TP
    offsets = jnp.arange(bound, dtype=jnp.int32)

    def one_expert(total, expert_id):
        positions = jnp.minimum(starts[expert_id] + offsets, assigned - 1).astype(jnp.int32)
        valid = (offsets < counts[expert_id]).astype(jnp.float32)
        picked = order[positions]
        token_ids = (picked // TOPK).astype(jnp.int32)
        rows_in = normed[token_ids]
        gate_pre = jnp.dot(rows_in, gate_w[expert_id], preferred_element_type=jnp.float32)
        up_pre = jnp.dot(rows_in, up_w[expert_id], preferred_element_type=jnp.float32)
        gate_act = jnp.minimum(gate_pre, 7.0)
        up_act = jnp.clip(up_pre, -7.0, 7.0)
        hidden = (gate_act * jax.nn.sigmoid(1.702 * gate_act) * (up_act + 1.0)).astype(jnp.bfloat16)
        expert_out = jnp.dot(hidden, down_w[expert_id], preferred_element_type=jnp.float32).astype(jnp.bfloat16)
        scaled = expert_out.astype(jnp.float32) * (flat_weight[picked] * valid)[:, None]
        return (total.at[token_ids].add(scaled), None)
    combined, _ = lax.scan(one_expert, jnp.zeros((length, D), jnp.float32), jnp.arange(EXPERTS, dtype=jnp.int32))
    return (stream.astype(jnp.float32) + rms_norm(combined, moe_gain)).astype(jnp.bfloat16)
```

```python
import jax
import jax.numpy as jnp
from jax import lax
from jax.experimental import pallas as pl
from jax.experimental.pallas import tpu as pltpu
from jax.sharding import PartitionSpec as P

EPS = 1e-06
F32 = jnp.float32
BF16 = jnp.bfloat16
MESH = pl.DeviceIdType.MESH
D = 2048
FF = 640
ROWS = 128
CAP = 16
HALF = ROWS // 2
COLS = 512
SOURCE_OF = (0, -1, 1, -2, 2, -3, 3, 4)
STEPS = ((0, 1), (1, 2), (3, 2), (5, 2), (7, 1))
MOVES = ((2, 0), (1, 0), (3, 0), (2, 1), (1, 1), (3, 1), (0, 1))


def rows_loop(count, size, fn):
    def step(i, carry):
        fn(pl.ds(pl.multiple_of(i * size, size), size))
        return carry

    lax.fori_loop(0, count, step, 0)


def kernel(
    b_ref, c_ref, v_ref, taps_ref, wproj_ref, resid_ref, post_ref, pre_ref, moe_ref, rw_ref,
    gw_ref, uw_ref, dw_ref,
    out_ref,
    wgu, dwv, edge, prodp, mixed, p0, p1, p3, x2, s1, s3, ra, rb, fm, fp,
    stream, xs, rwall, pmat, wmat, sel, rin, hid, eout, rback, part_u, part_d, su, sd, ru, rd,
    w_sem, e_ss, e_rs, rw_ss, rw_rs, x_ss, x_rs, ag_ss, ag_rs, d_ss, d_rs, r_ss, r_rs, z_ss, z_rs,
):
    sp = lax.axis_index("sp")
    tp = lax.axis_index("tp")
    z = sp // 8
    k = lax.rem(sp, 8)
    y = k // 2
    c = lax.rem(k, 2)

    def zdev(by):
        return {"sp": lax.rem(z + by + 8, 8) * 8 + k, "tp": tp}

    def in_plane(dy, dc):
        other = 1 - c if dc else c
        return lax.rem(y + dy + 4, 4) * 2 + other

    def pdev(index):
        return {"sp": z * 8 + index, "tp": tp}

    def xdev(by):
        return {"sp": sp, "tp": lax.rem(tp + by + 4, 4)}

    def sdev(by):
        return {"sp": lax.rem(sp + by + 64, 64), "tp": tp}

    def rcopy(src, dst, ss, rs, dev):
        return pltpu.make_async_remote_copy(
            src_ref=src, dst_ref=dst, send_sem=ss, recv_sem=rs, device_id=dev, device_id_type=MESH
        )

    weights = []
    for n in range(5):
        cols = pl.ds(n * 128, 128)
        weights.append(pltpu.make_async_copy(gw_ref.at[0, :, cols], wgu.at[n, :, pl.ds(0, 128)], w_sem.at[2 * n]))
        weights.append(pltpu.make_async_copy(uw_ref.at[0, :, cols], wgu.at[n, :, pl.ds(128, 128)], w_sem.at[2 * n + 1]))
    weights.append(pltpu.make_async_copy(dw_ref.at[0], dwv, w_sem.at[10]))
    for w in weights:
        w.start()

    barrier = pltpu.get_barrier_semaphore()
    peers = [xdev(1), xdev(2), xdev(3), sdev(1), sdev(-1)]
    peers += [zdev(by) for by in range(1, 8)]
    peers += [pdev(in_plane(dy, dc)) for dy, dc in MOVES]
    for dev in peers:
        pl.semaphore_signal(barrier, inc=1, device_id=dev, device_id_type=MESH)
    pl.semaphore_wait(barrier, len(peers))

    last = pl.ds(b_ref.shape[0] - 16, 16)
    edges = [
        rcopy(c_ref.at[last], edge.at[0], e_ss.at[0], e_rs.at[0], sdev(1)),
        rcopy(v_ref.at[last], edge.at[1], e_ss.at[1], e_rs.at[1], sdev(1)),
    ]
    for e in edges:
        e.start()
    routing = [
        rcopy(rw_ref, rwall.at[i], rw_ss.at[i], rw_rs.at[i], zdev(-SOURCE_OF[i])) for i in range(1, 8)
    ]
    for r in routing:
        r.start()
    rwall[0] = rw_ref[...]

    for i in range(4):
        rows = pl.ds(i * ROWS, ROWS)
        prodp[pl.ds(16 + i * ROWS, ROWS), :] = c_ref[rows, :].astype(F32) * v_ref[rows, :].astype(F32)
    for e in edges:
        e.wait_recv()
    prior = edge[0].astype(F32) * edge[1].astype(F32)
    prodp[0:16, :] = jnp.where(sp > 0, prior, jnp.zeros_like(prior))
    for i in range(4):
        at = i * ROWS
        filtered = (
            prodp[at + 14 : at + 14 + ROWS, :] * taps_ref[0:1, :]
            + prodp[at + 15 : at + 15 + ROWS, :] * taps_ref[1:2, :]
            + prodp[at + 16 : at + 16 + ROWS, :] * taps_ref[2:3, :]
        )
        mixed[at : at + ROWS, :] = (b_ref[at : at + ROWS, :].astype(F32) * filtered).astype(BF16)

    def project(by, dst):
        block = pl.ds(pl.multiple_of(lax.rem(tp + by, 4) * ROWS, ROWS), ROWS)

        def cols(at):
            got = jnp.dot(mixed[block, :], wproj_ref[:, at], preferred_element_type=F32)
            dst[:, at] = got.astype(dst.dtype)

        rows_loop(D // COLS, COLS, cols)

    lo, hi = pl.ds(0, HALF), pl.ds(HALF, HALF)

    project(2, x2)
    far_a = rcopy(x2.at[lo], ra, x_ss.at[0], x_rs.at[0], xdev(1))
    far_b = rcopy(x2.at[hi], rb, x_ss.at[1], x_rs.at[1], xdev(-1))
    far_a.start()
    far_b.start()
    project(1, p1)
    project(3, p3)

    def cast_rows(src, dst, base):
        def rows(at):
            dst[at, :] = src[at, :].astype(BF16)

        def step(i, carry):
            rows(pl.ds(pl.multiple_of(base + i * 16, 16), 16))
            return carry

        lax.fori_loop(0, HALF // 16, step, 0)

    def add_rows(src, more, shift, dst, base):
        def step(i, carry):
            at = pl.ds(pl.multiple_of(base + i * 16, 16), 16)
            there = pl.ds(pl.multiple_of(base - shift + i * 16, 16), 16)
            dst[at, :] = (src[at, :] + more[there, :].astype(F32)).astype(BF16)
            return carry

        lax.fori_loop(0, HALF // 16, step, 0)

    cast_rows(p1, s1, HALF)
    near_1b = rcopy(s1.at[hi], fm.at[hi], x_ss.at[2], x_rs.at[2], xdev(1))
    near_1b.start()
    cast_rows(p3, s3, 0)
    near_3a = rcopy(s3.at[lo], fp.at[lo], x_ss.at[3], x_rs.at[3], xdev(-1))
    near_3a.start()
    far_a.wait_recv()
    add_rows(p1, ra, 0, s1, 0)
    near_1a = rcopy(s1.at[lo], fm.at[lo], x_ss.at[4], x_rs.at[4], xdev(1))
    near_1a.start()
    far_b.wait_recv()
    add_rows(p3, rb, HALF, s3, HALF)
    near_3b = rcopy(s3.at[hi], fp.at[hi], x_ss.at[5], x_rs.at[5], xdev(-1))
    near_3b.start()
    project(0, p0)

    for r in routing:
        r.wait_recv()

    def tables(i, carry):
        rw = rwall[i]
        row = lax.broadcasted_iota(jnp.int32, (ROWS, ROWS), 0)
        lane = lax.broadcasted_iota(jnp.int32, (ROWS, ROWS), 1)
        expert = (z * 8 + row // CAP).astype(F32)
        slot = lax.rem(row, CAP).astype(F32)
        named = jnp.zeros((ROWS, ROWS), F32)
        weight = jnp.zeros((ROWS, ROWS), F32)
        for j in range(4):
            hit = rw[j : j + 1, :] == expert
            named = named + jnp.where(hit, 1.0, 0.0)
            weight = weight + jnp.where(hit, jnp.broadcast_to(rw[4 + j : 5 + j, :], (ROWS, ROWS)), 0.0)
        before = jnp.where(row < lane, 1.0, 0.0).astype(BF16)
        earlier = jnp.dot(named.astype(BF16), before, preferred_element_type=F32)
        picked = jnp.where(earlier == slot, named, 0.0)
        pmat[i] = picked.astype(BF16)
        wt = jnp.transpose(picked * weight)
        high = wt.astype(BF16)
        wmat[i, :, 0:ROWS] = high
        wmat[i, :, ROWS : 2 * ROWS] = (wt - high.astype(F32)).astype(BF16)
        return carry

    lax.fori_loop(0, 8, tables, 0)

    near_1b.wait_recv()
    near_1a.wait_recv()
    near_3a.wait_recv()
    near_3b.wait_recv()

    def norms(at):
        proj = p0[at, :] + fm[at, :].astype(F32) + fp[at, :].astype(F32)
        inv = lax.rsqrt(jnp.mean(proj * proj, axis=-1, keepdims=True) + EPS)
        st = (resid_ref[at, :].astype(F32) + proj * inv * post_ref[...]).astype(BF16)
        stream[at, :] = st
        wide = st.astype(F32)
        inv2 = lax.rsqrt(jnp.mean(wide * wide, axis=-1, keepdims=True) + EPS)
        xs[0, at, :] = (wide * inv2 * pre_ref[...]).astype(BF16)

    def ag(step, half, up):
        rows = lo if half == 0 else hi
        src = (0, 1, 3, 5) if up else (0, 2, 4, 6)
        dst = (1, 3, 5, 7) if up else (2, 4, 6, 7)
        at = (0 if up else 8) + 2 * step + half
        return rcopy(
            xs.at[src[step], rows], xs.at[dst[step], rows], ag_ss.at[at], ag_rs.at[at], zdev(1 if up else -1)
        )

    ring = {(s, h, u): ag(s, h, u) for s in range(3) for h in range(2) for u in (True, False)}
    ring[(3, 0, True)] = ag(3, 0, True)
    ring[(3, 1, False)] = ag(3, 1, False)

    for h in range(2):
        def half_rows(i, carry, h=h):
            norms(pl.ds(pl.multiple_of(h * HALF + i * 16, 16), 16))
            return carry

        lax.fori_loop(0, HALF // 16, half_rows, 0)
        ring[(0, h, True)].start()
        ring[(0, h, False)].start()

    def select(i):
        def cols(at):
            got = jnp.dot(pmat[i], xs[i, :, at], preferred_element_type=F32)
            sel[i, :, :, at] = got.astype(BF16).reshape(8, CAP, COLS)

        rows_loop(D // COLS, COLS, cols)

    def plane_sends(si, src, dst, ss, rs):
        first, n = STEPS[si]
        sends, waits = [], []
        for m, (dy, dc) in enumerate(MOVES):
            to = in_plane(dy, dc)
            frm = in_plane(-dy, dc)
            blocks = pl.ds(first, n)
            sends.append(rcopy(src.at[blocks, to], dst.at[blocks, k], ss.at[si, m], rs.at[si, m], pdev(to)))
            waits.append(rcopy(src.at[blocks, frm], dst.at[blocks, frm], ss.at[si, m], rs.at[si, m], pdev(to)))
        return sends, waits

    out_sends = [plane_sends(si, sel, rin, d_ss, d_rs) for si in range(5)]
    back_sends = [plane_sends(si, eout, rback, r_ss, r_rs) for si in range(5)]

    def dispatch(si):
        first, n = STEPS[si]
        for i in range(first, first + n):
            select(i)
        for s in out_sends[si][0]:
            s.start()
        for i in range(first, first + n):
            rin[i, k] = sel[i, k]

    def experts(si):
        first, n = STEPS[si]
        for w in out_sends[si][1]:
            w.wait_recv()
        if si == 0:
            for w in weights:
                w.wait()
        m = n * ROWS

        def gate_up(j, carry):
            x = rin[pl.ds(first, n)].reshape(m, D)
            gu = jnp.dot(x, wgu[j], preferred_element_type=F32)
            gate = jnp.minimum(gu[:, 0:128], 7.0)
            up = jnp.clip(gu[:, 128:256], -7.0, 7.0)
            hid[j, 0:m, :] = (gate * jax.nn.sigmoid(1.702 * gate) * (up + 1.0)).astype(BF16)
            return carry

        lax.fori_loop(0, 5, gate_up, 0)

        def down(at):
            h = jnp.concatenate([hid[j, 0:m, :] for j in range(5)], axis=1)
            got = jnp.dot(h, dwv[:, at], preferred_element_type=F32)
            eout[pl.ds(first, n), :, :, at] = got.astype(BF16).reshape(n, 8, CAP, COLS)

        rows_loop(D // COLS, COLS, down)

    dispatch(0)
    for s in range(1, 4):
        up_step, last_step = s - 1, s == 3
        for h in range(2):
            for u in (True, False):
                ring[(up_step, h, u)].wait_recv()
                if (s, h, u) in ring:
                    ring[(s, h, u)].start()
            if h == 0 and s >= 2:
                experts(s - 2)
        dispatch(s)
    experts(2)
    ring[(3, 0, True)].wait_recv()
    ring[(3, 1, False)].wait_recv()
    dispatch(4)
    experts(3)
    experts(4)

    for si in (4, 3, 2, 1, 0):
        first, n = STEPS[si]
        for s in back_sends[si][0]:
            s.start()
        for i in range(first, first + n):
            rback[i, k] = eout[i, k]

    def combine(i, dst):
        def cols(at):
            r = rback[i, :, :, at].reshape(ROWS, COLS)
            got = jnp.dot(wmat[i, :, 0:ROWS], r, preferred_element_type=F32)
            got = got + jnp.dot(wmat[i, :, ROWS : 2 * ROWS], r, preferred_element_type=F32)
            dst[:, at] = got.astype(dst.dtype)

        rows_loop(D // COLS, COLS, cols)

    def zsend(r, half, up):
        rows = lo if half == 0 else hi
        at = (0 if up else 8) + 2 * r + half
        src, dst = (su, ru) if up else (sd, rd)
        return rcopy(src.at[r, rows], dst.at[r, rows], z_ss.at[at], z_rs.at[at], zdev(1 if up else -1))

    back = {(r, h, u): zsend(r, h, u) for r in range(1, 4) for h in range(2) for u in (True, False)}
    back[(0, 0, True)] = zsend(0, 0, True)
    back[(0, 1, False)] = zsend(0, 1, False)

    for w in back_sends[4][1]:
        w.wait_recv()
    combine(7, part_u)
    cast_rows(part_u, su.at[0], 0)
    back[(0, 0, True)].start()
    cast_rows(part_u, sd.at[0], HALF)
    back[(0, 1, False)].start()
    for r, si in ((1, 3), (2, 2), (3, 1)):
        first, n = STEPS[si]
        for w in back_sends[si][1]:
            w.wait_recv()
        combine(first + 1, part_u)
        combine(first, part_d)
        for h, u in ((1, True), (0, False), (0, True), (1, False)):
            src, send, got = (part_u, su, ru) if u else (part_d, sd, rd)
            if (r - 1, h, u) in back:
                back[(r - 1, h, u)].wait_recv()
                add_rows(src, got.at[r - 1], 0, send.at[r], h * HALF)
            else:
                cast_rows(src, send.at[r], h * HALF)
            back[(r, h, u)].start()

    for w in back_sends[0][1]:
        w.wait_recv()
    combine(0, part_u)
    for h, u in ((1, True), (0, False), (0, True), (1, False)):
        back[(3, h, u)].wait_recv()

    def finish(at):
        total = part_u[at, :] + ru[3, at, :].astype(F32) + rd[3, at, :].astype(F32)
        inv = lax.rsqrt(jnp.mean(total * total, axis=-1, keepdims=True) + EPS)
        out_ref[at, :] = (stream[at, :].astype(F32) + total * inv * moe_ref[...]).astype(BF16)

    rows_loop(ROWS // 16, 16, finish)

    for s in edges + routing + [far_a, far_b, near_1a, near_1b, near_3a, near_3b]:
        s.wait_send()
    for s in list(ring.values()) + list(back.values()):
        s.wait_send()
    for sends, _ in out_sends + back_sends:
        for s in sends:
            s.wait_send()


def body(
    b_gate, c_gate, values_in, conv_taps, out_proj, resid, post_gain, pre_gain, moe_gain,
    routes, route_weight, gate_w, up_w, down_w,
):
    rw = jnp.concatenate([routes.astype(F32), route_weight], axis=1).T
    vmem = pl.BlockSpec(memory_space=pltpu.VMEM)
    hbm = pl.BlockSpec(memory_space=pl.ANY)
    dma = pltpu.SemaphoreType.DMA
    block = (ROWS, D)
    return pl.pallas_call(
        kernel,
        out_shape=jax.ShapeDtypeStruct(block, BF16),
        in_specs=[vmem] * 10 + [hbm] * 3,
        out_specs=vmem,
        scratch_shapes=[
            pltpu.VMEM((5, D, 256), BF16),
            pltpu.VMEM((FF, D), BF16),
            pltpu.VMEM((2, 16, 512), BF16),
            pltpu.VMEM((528, 512), F32),
            pltpu.VMEM((512, 512), BF16),
            pltpu.VMEM(block, F32),
            pltpu.VMEM(block, F32),
            pltpu.VMEM(block, F32),
            pltpu.VMEM(block, BF16),
            pltpu.VMEM(block, BF16),
            pltpu.VMEM(block, BF16),
            pltpu.VMEM((HALF, D), BF16),
            pltpu.VMEM((HALF, D), BF16),
            pltpu.VMEM(block, BF16),
            pltpu.VMEM(block, BF16),
            pltpu.VMEM(block, BF16),
            pltpu.VMEM((8,) + block, BF16),
            pltpu.VMEM((8, 8, 128), F32),
            pltpu.VMEM((8, ROWS, ROWS), BF16),
            pltpu.VMEM((8, ROWS, 2 * ROWS), BF16),
            pltpu.VMEM((8, 8, CAP, D), BF16),
            pltpu.VMEM((8, 8, CAP, D), BF16),
            pltpu.VMEM((5, 2 * ROWS, 128), BF16),
            pltpu.VMEM((8, 8, CAP, D), BF16),
            pltpu.VMEM((8, 8, CAP, D), BF16),
            pltpu.VMEM(block, F32),
            pltpu.VMEM(block, F32),
            pltpu.VMEM((4,) + block, BF16),
            pltpu.VMEM((4,) + block, BF16),
            pltpu.VMEM((4,) + block, BF16),
            pltpu.VMEM((4,) + block, BF16),
            dma((11,)),
            dma((2,)), dma((2,)),
            dma((8,)), dma((8,)),
            dma((6,)), dma((6,)),
            dma((16,)), dma((16,)),
            dma((5, 7)), dma((5, 7)),
            dma((5, 7)), dma((5, 7)),
            dma((16,)), dma((16,)),
        ],
        compiler_params=pltpu.CompilerParams(
            collective_id=0, has_side_effects=True, vmem_limit_bytes=63 * 2**20
        ),
    )(
        b_gate, c_gate, values_in, conv_taps, out_proj, resid,
        post_gain.reshape(1, D), pre_gain.reshape(1, D), moe_gain.reshape(1, D), rw,
        gate_w, up_w, down_w,
    )


def solution(mesh):
    rows = P(("sp", "tp"), None)
    placed = (
        P("sp", "tp"), P("sp", "tp"), P("sp", "tp"), P(None, "tp"), P("tp", None), rows,
        P(), P(), P(), rows, rows,
        P("sp", None, None), P("sp", None, None), P("sp", None, None),
    )
    return jax.shard_map(body, mesh=mesh, in_specs=placed, out_specs=rows, check_vma=False)
```

```python
import jax
import jax.numpy as jnp
from jax import lax
from jax.experimental import pallas as pl
from jax.experimental.pallas import tpu as pltpu
from jax.sharding import PartitionSpec as P

EPS = 1e-06
F32 = jnp.float32
BF16 = jnp.bfloat16
MESH = pl.DeviceIdType.MESH
D = 2048
FF = 640
ROWS = 128
CAP = 16
HALF = ROWS // 2
COLS = 512
SOURCE_OF = (0, -1, 1, -2, 2, -3, 3, 4)
STEPS = ((0, 1), (1, 2), (3, 2), (5, 2), (7, 1))
MOVES = ((2, 0), (1, 0), (3, 0), (2, 1), (1, 1), (3, 1), (0, 1))


def rows_loop(count, size, fn):
    def step(i, carry):
        fn(pl.ds(pl.multiple_of(i * size, size), size))
        return carry

    lax.fori_loop(0, count, step, 0)


def kernel(
    b_hbm, c_hbm, v_hbm, wproj_hbm, resid_hbm, taps_ref, post_ref, pre_ref, moe_ref, routes_ref, weight_ref,
    gw_ref, uw_ref, dw_ref,
    out_ref,
    b_ref, c_ref, v_ref, wproj_ref, resid_ref,
    wgu, dwv, edge, prodp, mixed, pj, x2, s1, s3, ra, rb, fm, fp,
    stream, xs, rwall, pmat, wmat, sel, rin, hid, eout, rback, part, sf, ss, rf, rs,
    l_sem, w_sem, e_ss, e_rs, rw_ss, rw_rs, x_ss, x_rs, ag_ss, ag_rs, d_ss, d_rs, r_ss, r_rs, z_ss, z_rs,
):
    sp = lax.axis_index("sp")
    tp = lax.axis_index("tp")
    z = sp // 8
    k = lax.rem(sp, 8)
    y = k // 2
    c = lax.rem(k, 2)

    def zdev(by):
        return {"sp": lax.rem(z + by + 8, 8) * 8 + k, "tp": tp}

    def other_core(dc):
        return 1 - c if dc else c

    def in_plane(dy, dc):
        return lax.rem(y + dy + 4, 4) * 2 + other_core(dc)

    def pdev(index):
        return {"sp": z * 8 + index, "tp": tp}

    def xdev(by):
        return {"sp": sp, "tp": lax.rem(tp + by + 4, 4)}

    def sdev(by):
        return {"sp": lax.rem(sp + by + 64, 64), "tp": tp}

    def rcopy(src, dst, ssem, rsem, dev):
        return pltpu.make_async_remote_copy(
            src_ref=src, dst_ref=dst, send_sem=ssem, recv_sem=rsem, device_id=dev, device_id_type=MESH
        )

    barrier = pltpu.get_barrier_semaphore()
    peers = [xdev(1), xdev(-1), sdev(1), sdev(-1)]
    peers += [zdev(by) for by in range(1, 8)]
    peers += [pdev(in_plane(dy, dc)) for dy, dc in MOVES]
    for dev in peers:
        pl.semaphore_signal(barrier, inc=1, device_id=dev, device_id_type=MESH)

    pairs = ((b_hbm, b_ref), (c_hbm, c_ref), (v_hbm, v_ref), (wproj_hbm, wproj_ref), (resid_hbm, resid_ref))
    loads = [pltpu.make_async_copy(src, dst, l_sem.at[i]) for i, (src, dst) in enumerate(pairs)]
    for i in (1, 2, 0, 3, 4):
        loads[i].start()
    weights = []
    for n in range(5):
        cols = pl.ds(n * 128, 128)
        weights.append(pltpu.make_async_copy(gw_ref.at[0, :, cols], wgu.at[n, :, pl.ds(0, 128)], w_sem.at[2 * n]))
        weights.append(pltpu.make_async_copy(uw_ref.at[0, :, cols], wgu.at[n, :, pl.ds(128, 128)], w_sem.at[2 * n + 1]))
    weights.append(pltpu.make_async_copy(dw_ref.at[0], dwv, w_sem.at[10]))
    for w in weights:
        w.start()

    rwall[0, 0:4, :] = routes_ref[...].astype(F32)
    rwall[0, 4:8, :] = weight_ref[...]

    prodp[0:16, :] = jnp.zeros((16, 512), F32)
    loads[1].wait()
    loads[2].wait()
    for i in range(4):
        rows = pl.ds(i * ROWS, ROWS)
        prodp[pl.ds(16 + i * ROWS, ROWS), :] = c_ref[rows, :].astype(F32) * v_ref[rows, :].astype(F32)
    loads[0].wait()

    def mix(at, count):
        filtered = (
            prodp[at + 14 : at + 14 + count, :] * taps_ref[0:1, :]
            + prodp[at + 15 : at + 15 + count, :] * taps_ref[1:2, :]
            + prodp[at + 16 : at + 16 + count, :] * taps_ref[2:3, :]
        )
        mixed[at : at + count, :] = (b_ref[at : at + count, :].astype(F32) * filtered).astype(BF16)

    for i in range(4):
        mix(i * ROWS, ROWS)
    loads[3].wait()

    def project(t, carry):
        rows = mixed[pl.ds(pl.multiple_of(t * ROWS, ROWS), ROWS), :]
        for n in range(4):
            got = jnp.dot(rows, wproj_ref[:, n * COLS : (n + 1) * COLS], preferred_element_type=F32)
            pj[t, n // 2, :, (n % 2) * COLS : (n % 2 + 1) * COLS] = got
        return carry

    lax.fori_loop(0, 4, project, 0)
    loads[4].wait()

    pl.semaphore_wait(barrier, len(peers))

    last = pl.ds(512 - 16, 16)
    edges = [
        rcopy(c_ref.at[last], edge.at[0], e_ss.at[0], e_rs.at[0], sdev(1)),
        rcopy(v_ref.at[last], edge.at[1], e_ss.at[1], e_rs.at[1], sdev(1)),
    ]
    for e in edges:
        e.start()

    lo, hi = pl.ds(0, HALF), pl.ds(HALF, HALF)
    halves = (lo, hi)
    t1, t2, t3 = lax.rem(tp + 1, 4), lax.rem(tp + 2, 4), lax.rem(tp + 3, 4)

    def put(t, ch, h, dst, more=None):
        def step(i, carry):
            at = pl.ds(pl.multiple_of(h * HALF + i * 16, 16), 16)
            val = pj[t, ch, at, :]
            if more is not None:
                val = val + more[at, :].astype(F32)
            dst[ch, at, :] = val.astype(BF16)
            return carry

        lax.fori_loop(0, HALF // 16, step, 0)

    x_sends = {}
    for h in range(2):
        rows = halves[h]
        i = 6 * h
        x_sends["far_a", h] = rcopy(x2.at[0, rows], ra.at[rows], x_ss.at[i], x_rs.at[i], xdev(1))
        x_sends["far_b", h] = rcopy(x2.at[1, rows], rb.at[rows], x_ss.at[i + 1], x_rs.at[i + 1], xdev(-1))
        x_sends["one_b", h] = rcopy(s1.at[1, rows], fm.at[1, rows], x_ss.at[i + 2], x_rs.at[i + 2], xdev(1))
        x_sends["three_a", h] = rcopy(s3.at[0, rows], fp.at[0, rows], x_ss.at[i + 3], x_rs.at[i + 3], xdev(-1))
        x_sends["one_a", h] = rcopy(s1.at[0, rows], fm.at[0, rows], x_ss.at[i + 4], x_rs.at[i + 4], xdev(1))
        x_sends["three_b", h] = rcopy(s3.at[1, rows], fp.at[1, rows], x_ss.at[i + 5], x_rs.at[i + 5], xdev(-1))

    def x_first(h):
        put(t2, 0, h, x2)
        x_sends["far_a", h].start()
        put(t2, 1, h, x2)
        x_sends["far_b", h].start()
        put(t1, 1, h, s1)
        x_sends["one_b", h].start()
        put(t3, 0, h, s3)
        x_sends["three_a", h].start()

    def x_second(h):
        x_sends["far_a", h].wait_recv()
        put(t1, 0, h, s1, ra)
        x_sends["one_a", h].start()
        x_sends["far_b", h].wait_recv()
        put(t3, 1, h, s3, rb)
        x_sends["three_b", h].start()

    x_first(1)
    routing = [
        rcopy(rwall.at[0], rwall.at[i], rw_ss.at[i], rw_rs.at[i], zdev(-SOURCE_OF[i])) for i in range(1, 8)
    ]
    for r in routing:
        r.start()
    for e in edges:
        e.wait_recv()
    prior = edge[0].astype(F32) * edge[1].astype(F32)
    prodp[0:16, :] = jnp.where(sp > 0, prior, jnp.zeros_like(prior))
    mix(0, 16)
    for n in range(4):
        got = jnp.dot(mixed[0:16, :], wproj_ref[:, n * COLS : (n + 1) * COLS], preferred_element_type=F32)
        pj[0, n // 2, 0:16, (n % 2) * COLS : (n % 2 + 1) * COLS] = got
    x_second(1)
    x_first(0)
    x_second(0)

    for r in routing:
        r.wait_recv()

    def tables(i, carry):
        rw = rwall[i]
        row = lax.broadcasted_iota(jnp.int32, (ROWS, ROWS), 0)
        lane = lax.broadcasted_iota(jnp.int32, (ROWS, ROWS), 1)
        expert = (z * 8 + row // CAP).astype(F32)
        slot = lax.rem(row, CAP).astype(F32)
        named = jnp.zeros((ROWS, ROWS), F32)
        weight = jnp.zeros((ROWS, ROWS), F32)
        for j in range(4):
            hit = rw[j : j + 1, :] == expert
            named = named + jnp.where(hit, 1.0, 0.0)
            weight = weight + jnp.where(hit, jnp.broadcast_to(rw[4 + j : 5 + j, :], (ROWS, ROWS)), 0.0)
        before = jnp.where(row < lane, 1.0, 0.0).astype(BF16)
        earlier = jnp.dot(named.astype(BF16), before, preferred_element_type=F32)
        picked = jnp.where(earlier == slot, named, 0.0)
        pmat[i] = picked.astype(BF16)
        wt = jnp.transpose(picked * weight)
        high = wt.astype(BF16)
        wmat[i, :, 0:ROWS] = high
        wmat[i, :, ROWS : 2 * ROWS] = (wt - high.astype(F32)).astype(BF16)
        return carry

    def ag(step, half, up):
        src = (0, 1, 3, 5) if up else (0, 2, 4, 6)
        dst = (1, 3, 5, 7) if up else (2, 4, 6, 7)
        at = (0 if up else 8) + 2 * step + half
        rows = halves[half]
        return rcopy(
            xs.at[src[step], rows], xs.at[dst[step], rows], ag_ss.at[at], ag_rs.at[at], zdev(1 if up else -1)
        )

    ring = {(s, h, u): ag(s, h, u) for s in range(3) for h in range(2) for u in (True, False)}
    ring[(3, 0, True)] = ag(3, 0, True)
    ring[(3, 1, False)] = ag(3, 1, False)

    wide = (slice(0, 1024), slice(1024, 2048))

    def norms(at):
        proj = [pj[tp, n, at, :] + fm[n, at, :].astype(F32) + fp[n, at, :].astype(F32) for n in range(2)]
        square = sum(jnp.sum(p * p, axis=-1, keepdims=True) for p in proj)
        inv = lax.rsqrt(square * (1.0 / D) + EPS)
        st = [
            (resid_ref[at, wide[n]].astype(F32) + proj[n] * inv * post_ref[:, wide[n]]).astype(BF16)
            for n in range(2)
        ]
        square = jnp.zeros_like(square)
        for n in range(2):
            stream[at, wide[n]] = st[n]
            st[n] = st[n].astype(F32)
            square = square + jnp.sum(st[n] * st[n], axis=-1, keepdims=True)
        inv2 = lax.rsqrt(square * (1.0 / D) + EPS)
        for n in range(2):
            xs[0, at, wide[n]] = (st[n] * inv2 * pre_ref[:, wide[n]]).astype(BF16)

    for h in (1, 0):
        for name in ("one_b", "three_a", "one_a", "three_b"):
            x_sends[name, h].wait_recv()

        def half_rows(i, carry, h=h):
            norms(pl.ds(pl.multiple_of(h * HALF + i * 16, 16), 16))
            return carry

        lax.fori_loop(0, HALF // 16, half_rows, 0)
        ring[(0, h, True)].start()
        ring[(0, h, False)].start()
        if h == 1:
            lax.fori_loop(0, 8, tables, 0)

    def select(i):
        def cols(at):
            got = jnp.dot(pmat[i], xs[i, :, at], preferred_element_type=F32)
            sel[i, :, :, at] = got.astype(BF16).reshape(8, CAP, COLS)

        rows_loop(D // COLS, COLS, cols)

    sent, arriving = {}, {}
    for si, (first, n) in enumerate(STEPS):
        blocks = pl.ds(first, n)
        for m, (dy, dc) in enumerate(MOVES):
            to, frm = in_plane(dy, dc), in_plane(-dy, dc)
            sem, rsem = d_ss.at[si, m], d_rs.at[si, m]
            sent[si, m] = rcopy(sel.at[blocks, to], rin.at[blocks, k], sem, rsem, pdev(to))
            arriving[si, m] = rcopy(sel.at[blocks, frm], rin.at[blocks, frm], sem, rsem, pdev(to))

    def dispatch(si):
        first, n = STEPS[si]
        for i in range(first, first + n):
            select(i)
        for m in range(7):
            sent[si, m].start()
        for i in range(first, first + n):
            rin[i, k] = sel[i, k]

    def experts(si):
        first, n = STEPS[si]
        for m in range(7):
            arriving[si, m].wait_recv()
        if si == 0:
            for w in weights:
                w.wait()
        m = n * ROWS

        def gate_up(j, carry):
            x = rin[pl.ds(first, n)].reshape(m, D)
            gu = jnp.dot(x, wgu[j], preferred_element_type=F32)
            gate = jnp.minimum(gu[:, 0:128], 7.0)
            up = jnp.clip(gu[:, 128:256], -7.0, 7.0)
            hid[j, 0:m, :] = (gate * jax.nn.sigmoid(1.702 * gate) * (up + 1.0)).astype(BF16)
            return carry

        lax.fori_loop(0, 5, gate_up, 0)

        def down(at):
            h = jnp.concatenate([hid[j, 0:m, :] for j in range(5)], axis=1)
            got = jnp.dot(h, dwv[:, at], preferred_element_type=F32)
            eout[pl.ds(first, n), :, :, at] = got.astype(BF16).reshape(n, 8, CAP, COLS)

        rows_loop(D // COLS, COLS, down)
        for i in range(first, first + n):
            rback[i, k] = eout[i, k]

    def block_of(slot, core):
        if slot == 0:
            return 7
        if slot == 7:
            return 0
        base = (5, 3, 1)[(slot - 1) // 2]
        return base + 1 - core if slot % 2 else base + core

    returned, coming = {}, {}
    for slot in range(8):
        for m, (dy, dc) in enumerate(MOVES):
            to, frm = in_plane(dy, dc), in_plane(-dy, dc)
            sem, rsem = r_ss.at[slot, m], r_rs.at[slot, m]
            theirs, mine = block_of(slot, other_core(dc)), block_of(slot, c)
            returned[slot, m] = rcopy(eout.at[theirs, to], rback.at[theirs, k], sem, rsem, pdev(to))
            coming[slot, m] = rcopy(eout.at[mine, frm], rback.at[mine, frm], sem, rsem, pdev(to))

    def send_back(slot):
        for m in range(7):
            returned[slot, m].start()

    dispatch(0)
    for s in range(1, 4):
        for h in (1, 0):
            for u in (True, False):
                ring[(s - 1, h, u)].wait_recv()
                if (s, h, u) in ring:
                    ring[(s, h, u)].start()
            if h == 1 and s >= 2:
                experts(s - 2)
        dispatch(s)
    experts(2)
    ring[(3, 0, True)].wait_recv()
    ring[(3, 1, False)].wait_recv()
    dispatch(4)
    send_back(7)
    experts(3)
    experts(4)
    for slot in range(7):
        send_back(slot)

    def combine(i, ch, dst, more=None):
        for n in range(2):
            at = slice(ch * 1024 + n * COLS, ch * 1024 + (n + 1) * COLS)
            here = slice(n * COLS, (n + 1) * COLS)
            r = rback[i, :, :, at].reshape(ROWS, COLS)
            got = jnp.dot(wmat[i, :, 0:ROWS], r, preferred_element_type=F32)
            got = got + jnp.dot(wmat[i, :, ROWS : 2 * ROWS], r, preferred_element_type=F32)
            if more is not None:
                got = got + more[:, here].astype(F32)
            dst[:, here] = got.astype(dst.dtype)

    def zsend(r, ch, f):
        at = (0 if f else 8) + 2 * r + ch
        src, dst = (sf, rf) if f else (ss, rs)
        return rcopy(src.at[r, ch], dst.at[r, ch], z_ss.at[at], z_rs.at[at], zdev(1 - 2 * c if f else 2 * c - 1))

    chain = {(r, ch, f): zsend(r, ch, f) for r in range(1, 4) for ch in range(2) for f in (True, False)}
    chain[(0, 0, True)] = zsend(0, 0, True)
    chain[(0, 1, False)] = zsend(0, 1, False)

    def take(slot):
        for m in range(7):
            coming[slot, m].wait_recv()

    take(7)
    combine(0, 0, part.at[0])
    combine(0, 1, part.at[1])
    take(0)
    combine(7, 0, sf.at[0, 0])
    chain[(0, 0, True)].start()
    combine(7, 1, ss.at[0, 1])
    chain[(0, 1, False)].start()
    for slot in range(1, 7):
        r, f = (slot + 1) // 2, slot % 2 == 1
        send, got = (sf, rf) if f else (ss, rs)
        take(slot)
        i = block_of(slot, c)
        for ch in ((1, 0) if f else (0, 1)):
            if (r - 1, ch, f) in chain:
                chain[(r - 1, ch, f)].wait_recv()
                combine(i, ch, send.at[r, ch], got.at[r - 1, ch])
            else:
                combine(i, ch, send.at[r, ch])
            chain[(r, ch, f)].start()

    for f, ch in ((True, 1), (True, 0), (False, 0), (False, 1)):
        chain[(3, ch, f)].wait_recv()

    def finish(at):
        total = [part[n, at, :] + rf[3, n, at, :].astype(F32) + rs[3, n, at, :].astype(F32) for n in range(2)]
        square = sum(jnp.sum(t * t, axis=-1, keepdims=True) for t in total)
        inv = lax.rsqrt(square * (1.0 / D) + EPS)
        for n in range(2):
            gained = total[n] * inv * moe_ref[:, wide[n]]
            out_ref[at, wide[n]] = (stream[at, wide[n]].astype(F32) + gained).astype(BF16)

    rows_loop(ROWS // 16, 16, finish)

    for group in (edges, routing, x_sends.values(), ring.values(), chain.values(), sent.values(), returned.values()):
        for s in group:
            s.wait_send()


def body(
    b_gate, c_gate, values_in, conv_taps, out_proj, resid, post_gain, pre_gain, moe_gain,
    routes, route_weight, gate_w, up_w, down_w,
):
    vmem = pl.BlockSpec(memory_space=pltpu.VMEM)
    hbm = pl.BlockSpec(memory_space=pl.ANY)
    dma = pltpu.SemaphoreType.DMA
    block = (ROWS, D)
    split = (2, ROWS, D // 2)
    return pl.pallas_call(
        kernel,
        out_shape=jax.ShapeDtypeStruct(block, BF16),
        in_specs=[hbm] * 5 + [vmem] * 6 + [hbm] * 3,
        out_specs=vmem,
        scratch_shapes=[
            pltpu.VMEM((512, 512), BF16),
            pltpu.VMEM((512, 512), BF16),
            pltpu.VMEM((512, 512), BF16),
            pltpu.VMEM((512, D), BF16),
            pltpu.VMEM(block, BF16),
            pltpu.VMEM((5, D, 256), BF16),
            pltpu.VMEM((FF, D), BF16),
            pltpu.VMEM((2, 16, 512), BF16),
            pltpu.VMEM((528, 512), F32),
            pltpu.VMEM((512, 512), BF16),
            pltpu.VMEM((4,) + split, F32),
            pltpu.VMEM(split, BF16),
            pltpu.VMEM(split, BF16),
            pltpu.VMEM(split, BF16),
            pltpu.VMEM((ROWS, D // 2), BF16),
            pltpu.VMEM((ROWS, D // 2), BF16),
            pltpu.VMEM(split, BF16),
            pltpu.VMEM(split, BF16),
            pltpu.VMEM(block, BF16),
            pltpu.VMEM((8,) + block, BF16),
            pltpu.VMEM((8, 8, 128), F32),
            pltpu.VMEM((8, ROWS, ROWS), BF16),
            pltpu.VMEM((8, ROWS, 2 * ROWS), BF16),
            pltpu.VMEM((8, 8, CAP, D), BF16),
            pltpu.VMEM((8, 8, CAP, D), BF16),
            pltpu.VMEM((5, 2 * ROWS, 128), BF16),
            pltpu.VMEM((8, 8, CAP, D), BF16),
            pltpu.VMEM((8, 8, CAP, D), BF16),
            pltpu.VMEM(split, F32),
            pltpu.VMEM((4,) + split, BF16),
            pltpu.VMEM((4,) + split, BF16),
            pltpu.VMEM((4,) + split, BF16),
            pltpu.VMEM((4,) + split, BF16),
            dma((5,)), dma((11,)),
            dma((2,)), dma((2,)),
            dma((8,)), dma((8,)),
            dma((12,)), dma((12,)),
            dma((16,)), dma((16,)),
            dma((5, 7)), dma((5, 7)),
            dma((8, 7)), dma((8, 7)),
            dma((16,)), dma((16,)),
        ],
        compiler_params=pltpu.CompilerParams(
            collective_id=0, has_side_effects=True, vmem_limit_bytes=63 * 2**20
        ),
    )(
        b_gate, c_gate, values_in, out_proj, resid, conv_taps,
        post_gain.reshape(1, D), pre_gain.reshape(1, D), moe_gain.reshape(1, D), routes.T, route_weight.T,
        gate_w, up_w, down_w,
    )


def solution(mesh):
    rows = P(("sp", "tp"), None)
    placed = (
        P("sp", "tp"), P("sp", "tp"), P("sp", "tp"), P(None, "tp"), P("tp", None), rows,
        P(), P(), P(), rows, rows,
        P("sp", None, None), P("sp", None, None), P("sp", None, None),
    )
    return jax.shard_map(body, mesh=mesh, in_specs=placed, out_specs=rows, check_vma=False)
```

```python
import jax
import jax.numpy as jnp
from jax import lax
from jax.experimental import pallas as pl
from jax.experimental.pallas import tpu as pltpu
from jax.sharding import PartitionSpec as P

EPS = 1e-06
F32 = jnp.float32
BF16 = jnp.bfloat16
MESH = pl.DeviceIdType.MESH
D = 2048
FF = 640
ROWS = 128
CAP = 16
HALF = ROWS // 2
COLS = 512
PARTED = (7, 1, 2, 3, 4, 5, 6)
MOVES = ((2, 0), (1, 0), (3, 0), (2, 1), (1, 1), (3, 1), (0, 1))


def rows_loop(count, size, fn):
    def step(i, carry):
        fn(pl.ds(pl.multiple_of(i * size, size), size))
        return carry

    lax.fori_loop(0, count, step, 0)


def kernel(
    b_hbm, c_hbm, v_hbm, wproj_hbm, resid_hbm, taps_ref, post_ref, pre_ref, moe_ref, routes_ref, weight_ref,
    gw_ref, uw_ref, dw_ref,
    out_ref,
    b_ref, c_ref, v_ref, wproj_ref, resid_ref,
    wgu, dwv, edge, prodp, mixed, pj, x2, s1, s3, ra, rb, fm, fp,
    stream, xs, rwall, pmat, wmat, sel, rin, hid, eout, rback, part, sf, ss, rf, rs,
    l_sem, w_sem, e_ss, e_rs, rw_ss, rw_rs, x_ss, x_rs, ag_ss, ag_rs, d_ss, d_rs, r_ss, r_rs, z_ss, z_rs,
):
    sp = lax.axis_index("sp")
    tp = lax.axis_index("tp")
    z = sp // 8
    k = lax.rem(sp, 8)
    y = k // 2
    c = lax.rem(k, 2)
    turn = 1 - 2 * c

    def zdev(by):
        return {"sp": lax.rem(z + by + 8, 8) * 8 + k, "tp": tp}

    def other_core(dc):
        return 1 - c if dc else c

    def in_plane(dy, dc):
        return lax.rem(y + dy + 4, 4) * 2 + other_core(dc)

    def pdev(index):
        return {"sp": z * 8 + index, "tp": tp}

    def xdev(by):
        return {"sp": sp, "tp": lax.rem(tp + by + 4, 4)}

    def sdev(by):
        return {"sp": lax.rem(sp + by + 64, 64), "tp": tp}

    def rcopy(src, dst, ssem, rsem, dev):
        return pltpu.make_async_remote_copy(
            src_ref=src, dst_ref=dst, send_sem=ssem, recv_sem=rsem, device_id=dev, device_id_type=MESH
        )

    barrier = pltpu.get_barrier_semaphore()
    peers = [xdev(1), xdev(-1), sdev(1), sdev(-1)]
    peers += [zdev(by) for by in range(1, 8)]
    peers += [pdev(in_plane(dy, dc)) for dy, dc in MOVES]
    for dev in peers:
        pl.semaphore_signal(barrier, inc=1, device_id=dev, device_id_type=MESH)

    pairs = ((b_hbm, b_ref), (c_hbm, c_ref), (v_hbm, v_ref), (wproj_hbm, wproj_ref), (resid_hbm, resid_ref))
    loads = [pltpu.make_async_copy(src, dst, l_sem.at[i]) for i, (src, dst) in enumerate(pairs)]
    for i in (1, 2, 0, 3, 4):
        loads[i].start()
    weights = []
    for n in range(5):
        cols = pl.ds(n * 128, 128)
        weights.append(pltpu.make_async_copy(gw_ref.at[0, :, cols], wgu.at[n, :, pl.ds(0, 128)], w_sem.at[2 * n]))
        weights.append(pltpu.make_async_copy(uw_ref.at[0, :, cols], wgu.at[n, :, pl.ds(128, 128)], w_sem.at[2 * n + 1]))
    weights.append(pltpu.make_async_copy(dw_ref.at[0], dwv, w_sem.at[10]))
    for w in weights:
        w.start()

    rwall[0, 0:4, :] = routes_ref[...].astype(F32)
    rwall[0, 4:8, :] = weight_ref[...]

    prodp[0:16, :] = jnp.zeros((16, 512), F32)
    loads[1].wait()
    loads[2].wait()
    for i in range(4):
        rows = pl.ds(i * ROWS, ROWS)
        prodp[pl.ds(16 + i * ROWS, ROWS), :] = c_ref[rows, :].astype(F32) * v_ref[rows, :].astype(F32)
    loads[0].wait()

    def mix(at, count):
        filtered = (
            prodp[at + 14 : at + 14 + count, :] * taps_ref[0:1, :]
            + prodp[at + 15 : at + 15 + count, :] * taps_ref[1:2, :]
            + prodp[at + 16 : at + 16 + count, :] * taps_ref[2:3, :]
        )
        mixed[at : at + count, :] = (b_ref[at : at + count, :].astype(F32) * filtered).astype(BF16)

    for i in range(4):
        mix(i * ROWS, ROWS)
    loads[3].wait()

    def project(t, carry):
        rows = mixed[pl.ds(pl.multiple_of(t * ROWS, ROWS), ROWS), :]
        for n in range(4):
            got = jnp.dot(rows, wproj_ref[:, n * COLS : (n + 1) * COLS], preferred_element_type=F32)
            pj[t, n // 2, :, (n % 2) * COLS : (n % 2 + 1) * COLS] = got
        return carry

    lax.fori_loop(0, 4, project, 0)
    loads[4].wait()

    pl.semaphore_wait(barrier, len(peers))

    last = pl.ds(512 - 16, 16)
    edges = [
        rcopy(c_ref.at[last], edge.at[0], e_ss.at[0], e_rs.at[0], sdev(1)),
        rcopy(v_ref.at[last], edge.at[1], e_ss.at[1], e_rs.at[1], sdev(1)),
    ]
    for e in edges:
        e.start()

    lo, hi = pl.ds(0, HALF), pl.ds(HALF, HALF)
    halves = (lo, hi)
    t1, t2, t3 = lax.rem(tp + 1, 4), lax.rem(tp + 2, 4), lax.rem(tp + 3, 4)

    def put(t, ch, h, dst, more=None):
        def step(i, carry):
            at = pl.ds(pl.multiple_of(h * HALF + i * 16, 16), 16)
            val = pj[t, ch, at, :]
            if more is not None:
                val = val + more[at, :].astype(F32)
            dst[ch, at, :] = val.astype(BF16)
            return carry

        lax.fori_loop(0, HALF // 16, step, 0)

    x_sends = {}
    for h in range(2):
        rows = halves[h]
        i = 6 * h
        x_sends["far_a", h] = rcopy(x2.at[0, rows], ra.at[rows], x_ss.at[i], x_rs.at[i], xdev(1))
        x_sends["far_b", h] = rcopy(x2.at[1, rows], rb.at[rows], x_ss.at[i + 1], x_rs.at[i + 1], xdev(-1))
        x_sends["one_b", h] = rcopy(s1.at[1, rows], fm.at[1, rows], x_ss.at[i + 2], x_rs.at[i + 2], xdev(1))
        x_sends["three_a", h] = rcopy(s3.at[0, rows], fp.at[0, rows], x_ss.at[i + 3], x_rs.at[i + 3], xdev(-1))
        x_sends["one_a", h] = rcopy(s1.at[0, rows], fm.at[0, rows], x_ss.at[i + 4], x_rs.at[i + 4], xdev(1))
        x_sends["three_b", h] = rcopy(s3.at[1, rows], fp.at[1, rows], x_ss.at[i + 5], x_rs.at[i + 5], xdev(-1))

    def x_far(h):
        put(t2, 0, h, x2)
        x_sends["far_a", h].start()
        put(t2, 1, h, x2)
        x_sends["far_b", h].start()

    def x_near(h):
        put(t1, 1, h, s1)
        x_sends["one_b", h].start()
        put(t3, 0, h, s3)
        x_sends["three_a", h].start()

    def x_second(h):
        x_sends["far_a", h].wait_recv()
        put(t1, 0, h, s1, ra)
        x_sends["one_a", h].start()
        x_sends["far_b", h].wait_recv()
        put(t3, 1, h, s3, rb)
        x_sends["three_b", h].start()

    x_far(1)
    x_near(1)
    routing = [
        rcopy(rwall.at[0], rwall.at[i], rw_ss.at[i], rw_rs.at[i], zdev(turn * ((i + 1) // 2) * (1 if i % 2 else -1)))
        for i in range(1, 8)
    ]
    for r in routing:
        r.start()
    for e in edges:
        e.wait_recv()
    prior = edge[0].astype(F32) * edge[1].astype(F32)
    prodp[0:16, :] = jnp.where(sp > 0, prior, jnp.zeros_like(prior))
    mix(0, 16)
    for n in range(4):
        got = jnp.dot(mixed[0:16, :], wproj_ref[:, n * COLS : (n + 1) * COLS], preferred_element_type=F32)
        pj[0, n // 2, 0:16, (n % 2) * COLS : (n % 2 + 1) * COLS] = got
    x_far(0)
    x_second(1)
    x_near(0)

    for r in routing:
        r.wait_recv()

    def tables(i, carry):
        rw = rwall[i]
        row = lax.broadcasted_iota(jnp.int32, (ROWS, ROWS), 0)
        lane = lax.broadcasted_iota(jnp.int32, (ROWS, ROWS), 1)
        expert = (z * 8 + row // CAP).astype(F32)
        slot = lax.rem(row, CAP).astype(F32)
        named = jnp.zeros((ROWS, ROWS), F32)
        weight = jnp.zeros((ROWS, ROWS), F32)
        for j in range(4):
            hit = rw[j : j + 1, :] == expert
            named = named + jnp.where(hit, 1.0, 0.0)
            weight = weight + jnp.where(hit, jnp.broadcast_to(rw[4 + j : 5 + j, :], (ROWS, ROWS)), 0.0)
        before = jnp.where(row < lane, 1.0, 0.0).astype(BF16)
        earlier = jnp.dot(named.astype(BF16), before, preferred_element_type=F32)
        picked = jnp.where(earlier == slot, named, 0.0)
        pmat[i] = picked.astype(BF16)
        wt = jnp.transpose(picked * weight)
        high = wt.astype(BF16)
        wmat[i, :, 0:ROWS] = high
        wmat[i, :, ROWS : 2 * ROWS] = (wt - high.astype(F32)).astype(BF16)
        return carry

    lax.fori_loop(0, 8, tables, 0)
    x_second(0)

    def ag(step, half, f):
        src = 0 if step == 0 else 2 * step - 1 if f else 2 * step
        dst = min(2 * step + 1 if f else 2 * step + 2, 7)
        at = (0 if f else 8) + 2 * step + half
        rows = halves[half]
        return rcopy(xs.at[src, rows], xs.at[dst, rows], ag_ss.at[at], ag_rs.at[at], zdev(turn if f else -turn))

    ring = {(s, h, f): ag(s, h, f) for s in range(3) for h in range(2) for f in (True, False)}
    ring[(3, 1, True)] = ag(3, 1, True)
    ring[(3, 0, False)] = ag(3, 0, False)

    def forward(step, half, f):
        ring[(step - 1, half, f)].wait_recv()
        if (step, half, f) in ring:
            ring[(step, half, f)].start()

    wide = (slice(0, 1024), slice(1024, 2048))

    def norms(at):
        proj = [pj[tp, n, at, :] + fm[n, at, :].astype(F32) + fp[n, at, :].astype(F32) for n in range(2)]
        square = sum(jnp.sum(p * p, axis=-1, keepdims=True) for p in proj)
        inv = lax.rsqrt(square * (1.0 / D) + EPS)
        st = [
            (resid_ref[at, wide[n]].astype(F32) + proj[n] * inv * post_ref[:, wide[n]]).astype(BF16)
            for n in range(2)
        ]
        square = jnp.zeros_like(square)
        for n in range(2):
            stream[at, wide[n]] = st[n]
            st[n] = st[n].astype(F32)
            square = square + jnp.sum(st[n] * st[n], axis=-1, keepdims=True)
        inv2 = lax.rsqrt(square * (1.0 / D) + EPS)
        for n in range(2):
            xs[0, at, wide[n]] = (st[n] * inv2 * pre_ref[:, wide[n]]).astype(BF16)

    def normed_rows(h):
        for name in ("one_b", "three_a", "one_a", "three_b"):
            x_sends[name, h].wait_recv()

        def half_rows(i, carry):
            norms(pl.ds(pl.multiple_of(h * HALF + i * 16, 16), 16))
            return carry

        lax.fori_loop(0, HALF // 16, half_rows, 0)

    def select(i):
        def cols(at):
            got = jnp.dot(pmat[i], xs[i, :, at], preferred_element_type=F32)
            sel[i, :, :, at] = got.astype(BF16).reshape(8, CAP, COLS)

        rows_loop(D // COLS, COLS, cols)

    sent, arriving, returned, coming = {}, {}, {}, {}
    for slot in range(8):
        for m, (dy, dc) in enumerate(MOVES):
            to, frm = in_plane(dy, dc), in_plane(-dy, dc)
            sems = d_ss.at[slot, m], d_rs.at[slot, m]
            sent[slot, m] = rcopy(sel.at[slot, to], rin.at[slot, k], *sems, pdev(to))
            arriving[slot, m] = rcopy(sel.at[slot, frm], rin.at[slot, frm], *sems, pdev(to))
            for ch in (0, 1) if slot in PARTED else (0,):
                cols = pl.ds(1024 * ch, 1024 if slot in PARTED else D)
                sems = r_ss.at[slot + 8 * ch, m], r_rs.at[slot + 8 * ch, m]
                returned[slot, ch, m] = rcopy(eout.at[slot, to, :, cols], rback.at[slot, k, :, cols], *sems, pdev(to))
                coming[slot, ch, m] = rcopy(eout.at[slot, frm, :, cols], rback.at[slot, frm, :, cols], *sems, pdev(to))

    def dispatch(slot):
        for m in range(7):
            sent[slot, m].start()
        rin[slot, k] = sel[slot, k]

    def send_back(slot, ch=0):
        for m in range(7):
            returned[slot, ch, m].start()

    def order_of(slot):
        return (1, 0) if slot % 2 == 1 else (0, 1)

    def experts(first, n, parted=False):
        for i in range(first, first + n):
            for m in range(7):
                arriving[i, m].wait_recv()
        if first == 0:
            for w in weights:
                w.wait()
        m = n * ROWS

        def gate_up(j, carry):
            x = rin[pl.ds(first, n)].reshape(m, D)
            gu = jnp.dot(x, wgu[j], preferred_element_type=F32)
            gate = jnp.minimum(gu[:, 0:128], 7.0)
            up = jnp.clip(gu[:, 128:256], -7.0, 7.0)
            hid[j, 0:m, :] = (gate * jax.nn.sigmoid(1.702 * gate) * (up + 1.0)).astype(BF16)
            return carry

        lax.fori_loop(0, 5, gate_up, 0)

        def down(at):
            h = jnp.concatenate([hid[j, 0:m, :] for j in range(5)], axis=1)
            got = jnp.dot(h, dwv[:, at], preferred_element_type=F32)
            eout[pl.ds(first, n), :, :, at] = got.astype(BF16).reshape(n, 8, CAP, COLS)

        if parted:
            for half in range(2):
                for n_ in range(2):
                    down(pl.ds(half * 1024 + n_ * COLS, COLS))
                send_back(7, half)
        else:
            rows_loop(D // COLS, COLS, down)
        for i in range(first, first + n):
            rback[i, k] = eout[i, k]

    normed_rows(1)
    ring[(0, 1, True)].start()
    ring[(0, 1, False)].start()
    normed_rows(0)
    ring[(0, 0, True)].start()
    select(0)
    dispatch(0)
    ring[(0, 0, False)].start()
    forward(1, 1, True)
    forward(1, 1, False)
    forward(1, 0, True)
    select(1)
    dispatch(1)
    forward(1, 0, False)
    select(2)
    dispatch(2)
    experts(0, 1)
    forward(2, 1, True)
    forward(2, 0, True)
    select(3)
    dispatch(3)
    forward(2, 1, False)
    forward(2, 0, False)
    select(4)
    dispatch(4)
    experts(1, 2)
    forward(3, 1, True)
    forward(3, 0, True)
    select(5)
    dispatch(5)
    forward(3, 0, False)
    forward(3, 1, False)
    select(6)
    ring[(3, 1, True)].wait_recv()
    ring[(3, 0, False)].wait_recv()
    select(7)
    dispatch(7)
    dispatch(6)
    experts(3, 2)
    experts(5, 1)
    experts(7, 1, True)
    for ch in order_of(5) if 5 in PARTED else (0,):
        send_back(5, ch)
    experts(6, 1)
    for slot in (6, 3, 4, 1, 2, 0):
        for ch in order_of(slot) if slot in PARTED else (0,):
            send_back(slot, ch)

    def combine(i, ch, dst, more=None):
        for n in range(2):
            at = slice(ch * 1024 + n * COLS, ch * 1024 + (n + 1) * COLS)
            here = slice(n * COLS, (n + 1) * COLS)
            r = rback[i, :, :, at].reshape(ROWS, COLS)
            got = jnp.dot(wmat[i, :, 0:ROWS], r, preferred_element_type=F32)
            got = got + jnp.dot(wmat[i, :, ROWS : 2 * ROWS], r, preferred_element_type=F32)
            if more is not None:
                got = got + more[:, here].astype(F32)
            dst[:, here] = got.astype(dst.dtype)

    def zsend(r, ch, f):
        at = (0 if f else 8) + 2 * r + ch
        src, dst = (sf, rf) if f else (ss, rs)
        return rcopy(src.at[r, ch], dst.at[r, ch], z_ss.at[at], z_rs.at[at], zdev(-turn if f else turn))

    chain = {(r, ch, f): zsend(r, ch, f) for r in range(1, 4) for ch in range(2) for f in (True, False)}
    chain[(0, 0, True)] = zsend(0, 0, True)
    chain[(0, 1, False)] = zsend(0, 1, False)

    def take(slot, ch=0):
        for m in range(7):
            coming[slot, ch, m].wait_recv()

    take(7)
    combine(7, 0, sf.at[0, 0])
    chain[(0, 0, True)].start()
    take(7, 1)
    combine(7, 1, ss.at[0, 1])
    chain[(0, 1, False)].start()
    for slot in (5, 6, 3, 4, 1, 2):
        f = slot % 2 == 1
        r = 4 - (slot + 1) // 2
        send, got = (sf, rf) if f else (ss, rs)
        if slot not in PARTED:
            take(slot)
        for ch in order_of(slot):
            if slot in PARTED:
                take(slot, ch)
            if (r - 1, ch, f) in chain:
                chain[(r - 1, ch, f)].wait_recv()
                combine(slot, ch, send.at[r, ch], got.at[r - 1, ch])
            else:
                combine(slot, ch, send.at[r, ch])
            chain[(r, ch, f)].start()

    take(0)
    combine(0, 0, part.at[0])
    combine(0, 1, part.at[1])
    for f, ch in ((True, 1), (True, 0), (False, 0), (False, 1)):
        chain[(3, ch, f)].wait_recv()

    def finish(at):
        total = [part[n, at, :] + rf[3, n, at, :].astype(F32) + rs[3, n, at, :].astype(F32) for n in range(2)]
        square = sum(jnp.sum(t * t, axis=-1, keepdims=True) for t in total)
        inv = lax.rsqrt(square * (1.0 / D) + EPS)
        for n in range(2):
            gained = total[n] * inv * moe_ref[:, wide[n]]
            out_ref[at, wide[n]] = (stream[at, wide[n]].astype(F32) + gained).astype(BF16)

    rows_loop(ROWS // 16, 16, finish)

    late = [ring[key] for key in ring]
    for group in (edges, routing, x_sends.values(), late, chain.values(), sent.values(), returned.values()):
        for s in group:
            s.wait_send()


def body(
    b_gate, c_gate, values_in, conv_taps, out_proj, resid, post_gain, pre_gain, moe_gain,
    routes, route_weight, gate_w, up_w, down_w,
):
    vmem = pl.BlockSpec(memory_space=pltpu.VMEM)
    hbm = pl.BlockSpec(memory_space=pl.ANY)
    dma = pltpu.SemaphoreType.DMA
    block = (ROWS, D)
    split = (2, ROWS, D // 2)
    return pl.pallas_call(
        kernel,
        out_shape=jax.ShapeDtypeStruct(block, BF16),
        in_specs=[hbm] * 5 + [vmem] * 6 + [hbm] * 3,
        out_specs=vmem,
        scratch_shapes=[
            pltpu.VMEM((512, 512), BF16),
            pltpu.VMEM((512, 512), BF16),
            pltpu.VMEM((512, 512), BF16),
            pltpu.VMEM((512, D), BF16),
            pltpu.VMEM(block, BF16),
            pltpu.VMEM((5, D, 256), BF16),
            pltpu.VMEM((FF, D), BF16),
            pltpu.VMEM((2, 16, 512), BF16),
            pltpu.VMEM((528, 512), F32),
            pltpu.VMEM((512, 512), BF16),
            pltpu.VMEM((4,) + split, F32),
            pltpu.VMEM(split, BF16),
            pltpu.VMEM(split, BF16),
            pltpu.VMEM(split, BF16),
            pltpu.VMEM((ROWS, D // 2), BF16),
            pltpu.VMEM((ROWS, D // 2), BF16),
            pltpu.VMEM(split, BF16),
            pltpu.VMEM(split, BF16),
            pltpu.VMEM(block, BF16),
            pltpu.VMEM((8,) + block, BF16),
            pltpu.VMEM((8, 8, 128), F32),
            pltpu.VMEM((8, ROWS, ROWS), BF16),
            pltpu.VMEM((8, ROWS, 2 * ROWS), BF16),
            pltpu.VMEM((8, 8, CAP, D), BF16),
            pltpu.VMEM((8, 8, CAP, D), BF16),
            pltpu.VMEM((5, 2 * ROWS, 128), BF16),
            pltpu.VMEM((8, 8, CAP, D), BF16),
            pltpu.VMEM((8, 8, CAP, D), BF16),
            pltpu.VMEM(split, F32),
            pltpu.VMEM((4,) + split, BF16),
            pltpu.VMEM((4,) + split, BF16),
            pltpu.VMEM((4,) + split, BF16),
            pltpu.VMEM((4,) + split, BF16),
            dma((5,)), dma((11,)),
            dma((2,)), dma((2,)),
            dma((8,)), dma((8,)),
            dma((12,)), dma((12,)),
            dma((16,)), dma((16,)),
            dma((8, 7)), dma((8, 7)),
            dma((16, 7)), dma((16, 7)),
            dma((16,)), dma((16,)),
        ],
        compiler_params=pltpu.CompilerParams(
            collective_id=0, has_side_effects=True, vmem_limit_bytes=63 * 2**20
        ),
    )(
        b_gate, c_gate, values_in, out_proj, resid, conv_taps,
        post_gain.reshape(1, D), pre_gain.reshape(1, D), moe_gain.reshape(1, D), routes.T, route_weight.T,
        gate_w, up_w, down_w,
    )


def solution(mesh):
    rows = P(("sp", "tp"), None)
    placed = (
        P("sp", "tp"), P("sp", "tp"), P("sp", "tp"), P(None, "tp"), P("tp", None), rows,
        P(), P(), P(), rows, rows,
        P("sp", None, None), P("sp", None, None), P("sp", None, None),
    )
    return jax.shard_map(body, mesh=mesh, in_specs=placed, out_specs=rows, check_vma=False)
```

```python
import jax
import jax.numpy as jnp
from jax import lax
from jax.experimental import pallas as pl
from jax.experimental.pallas import tpu as pltpu
from jax.sharding import PartitionSpec as P

EPS = 1e-06
F32 = jnp.float32
BF16 = jnp.bfloat16
MESH = pl.DeviceIdType.MESH
D = 2048
FF = 640
ROWS = 128
CAP = 16
HALF = ROWS // 2
COLS = 512
PARTED = (7, 1, 2, 3, 4, 5, 6)
MOVES = ((2, 0), (1, 0), (3, 0), (2, 1), (1, 1), (3, 1), (0, 1))


def rows_loop(count, size, fn):
    def step(i, carry):
        fn(pl.ds(pl.multiple_of(i * size, size), size))
        return carry

    lax.fori_loop(0, count, step, 0)


def kernel(
    b_hbm, c_hbm, v_hbm, wproj_hbm, resid_hbm, taps_ref, post_ref, pre_ref, moe_ref, routes_ref, weight_ref,
    gw_ref, uw_ref, dw_ref,
    out_ref,
    b_ref, c_ref, v_ref, wproj_ref, resid_ref,
    wgu, dwv, edge, prodp, mixed, pj, x2, s1, s3, ra, rb, fm, fp,
    stream, xs, rwall, pmat, wmat, sel, rin, hid, eout, rback, part, sf, ss, rf, rs,
    l_sem, w_sem, e_ss, e_rs, rw_ss, rw_rs, x_ss, x_rs, ag_ss, ag_rs, d_ss, d_rs, r_ss, r_rs, z_ss, z_rs,
):
    sp = lax.axis_index("sp")
    tp = lax.axis_index("tp")
    z = sp // 8
    k = lax.rem(sp, 8)
    y = k // 2
    c = lax.rem(k, 2)
    turn = 1 - 2 * c

    def zdev(by):
        return {"sp": lax.rem(z + by + 8, 8) * 8 + k, "tp": tp}

    def other_core(dc):
        return 1 - c if dc else c

    def in_plane(dy, dc):
        return lax.rem(y + dy + 4, 4) * 2 + other_core(dc)

    def pdev(index):
        return {"sp": z * 8 + index, "tp": tp}

    def xdev(by):
        return {"sp": sp, "tp": lax.rem(tp + by + 4, 4)}

    def sdev(by):
        return {"sp": lax.rem(sp + by + 64, 64), "tp": tp}

    def rcopy(src, dst, ssem, rsem, dev):
        return pltpu.make_async_remote_copy(
            src_ref=src, dst_ref=dst, send_sem=ssem, recv_sem=rsem, device_id=dev, device_id_type=MESH
        )

    barrier = pltpu.get_barrier_semaphore()
    peers = [xdev(1), xdev(-1), sdev(1), sdev(-1)]
    peers += [zdev(by) for by in range(1, 8)]
    peers += [pdev(in_plane(dy, dc)) for dy, dc in MOVES]
    for dev in peers:
        pl.semaphore_signal(barrier, inc=1, device_id=dev, device_id_type=MESH)

    pairs = ((b_hbm, b_ref), (c_hbm, c_ref), (v_hbm, v_ref), (wproj_hbm, wproj_ref), (resid_hbm, resid_ref))
    loads = [pltpu.make_async_copy(src, dst, l_sem.at[i]) for i, (src, dst) in enumerate(pairs)]
    for i in (1, 2, 0, 3, 4):
        loads[i].start()
    weights = []
    for n in range(5):
        cols = pl.ds(n * 128, 128)
        weights.append(pltpu.make_async_copy(gw_ref.at[0, :, cols], wgu.at[n, :, pl.ds(0, 128)], w_sem.at[2 * n]))
        weights.append(pltpu.make_async_copy(uw_ref.at[0, :, cols], wgu.at[n, :, pl.ds(128, 128)], w_sem.at[2 * n + 1]))
    weights.append(pltpu.make_async_copy(dw_ref.at[0], dwv, w_sem.at[10]))
    for w in weights:
        w.start()

    rwall[0, 0:4, :] = routes_ref[...].astype(F32)
    rwall[0, 4:8, :] = weight_ref[...]

    prodp[0:16, :] = jnp.zeros((16, 512), F32)
    loads[1].wait()
    loads[2].wait()
    for i in range(4):
        rows = pl.ds(i * ROWS, ROWS)
        prodp[pl.ds(16 + i * ROWS, ROWS), :] = c_ref[rows, :].astype(F32) * v_ref[rows, :].astype(F32)
    loads[0].wait()

    def mix(at, count):
        filtered = (
            prodp[at + 14 : at + 14 + count, :] * taps_ref[0:1, :]
            + prodp[at + 15 : at + 15 + count, :] * taps_ref[1:2, :]
            + prodp[at + 16 : at + 16 + count, :] * taps_ref[2:3, :]
        )
        mixed[at : at + count, :] = (b_ref[at : at + count, :].astype(F32) * filtered).astype(BF16)

    for i in range(4):
        mix(i * ROWS, ROWS)
    loads[3].wait()

    def project(t, carry):
        rows = mixed[pl.ds(pl.multiple_of(t * ROWS, ROWS), ROWS), :]
        for n in range(4):
            got = jnp.dot(rows, wproj_ref[:, n * COLS : (n + 1) * COLS], preferred_element_type=F32)
            pj[t, n // 2, :, (n % 2) * COLS : (n % 2 + 1) * COLS] = got
        return carry

    lax.fori_loop(0, 4, project, 0)
    loads[4].wait()

    pl.semaphore_wait(barrier, len(peers))

    last = pl.ds(512 - 16, 16)
    edges = [
        rcopy(c_ref.at[last], edge.at[0], e_ss.at[0], e_rs.at[0], sdev(1)),
        rcopy(v_ref.at[last], edge.at[1], e_ss.at[1], e_rs.at[1], sdev(1)),
    ]
    for e in edges:
        e.start()

    lo, hi = pl.ds(0, HALF), pl.ds(HALF, HALF)
    halves = (lo, hi)
    t1, t2, t3 = lax.rem(tp + 1, 4), lax.rem(tp + 2, 4), lax.rem(tp + 3, 4)

    def put(t, ch, h, dst, more=None):
        def step(i, carry):
            at = pl.ds(pl.multiple_of(h * HALF + i * 16, 16), 16)
            val = pj[t, ch, at, :]
            if more is not None:
                val = val + more[at, :].astype(F32)
            dst[ch, at, :] = val.astype(BF16)
            return carry

        lax.fori_loop(0, HALF // 16, step, 0)

    x_sends = {}
    for h in range(2):
        rows = halves[h]
        i = 6 * h
        x_sends["far_a", h] = rcopy(x2.at[0, rows], ra.at[rows], x_ss.at[i], x_rs.at[i], xdev(1))
        x_sends["far_b", h] = rcopy(x2.at[1, rows], rb.at[rows], x_ss.at[i + 1], x_rs.at[i + 1], xdev(-1))
        x_sends["one_b", h] = rcopy(s1.at[1, rows], fm.at[1, rows], x_ss.at[i + 2], x_rs.at[i + 2], xdev(1))
        x_sends["three_a", h] = rcopy(s3.at[0, rows], fp.at[0, rows], x_ss.at[i + 3], x_rs.at[i + 3], xdev(-1))
        x_sends["one_a", h] = rcopy(s1.at[0, rows], fm.at[0, rows], x_ss.at[i + 4], x_rs.at[i + 4], xdev(1))
        x_sends["three_b", h] = rcopy(s3.at[1, rows], fp.at[1, rows], x_ss.at[i + 5], x_rs.at[i + 5], xdev(-1))

    def x_far(h):
        put(t2, 0, h, x2)
        x_sends["far_a", h].start()
        put(t2, 1, h, x2)
        x_sends["far_b", h].start()

    def x_near(h):
        put(t1, 1, h, s1)
        x_sends["one_b", h].start()
        put(t3, 0, h, s3)
        x_sends["three_a", h].start()

    def x_second(h):
        x_sends["far_a", h].wait_recv()
        put(t1, 0, h, s1, ra)
        x_sends["one_a", h].start()
        x_sends["far_b", h].wait_recv()
        put(t3, 1, h, s3, rb)
        x_sends["three_b", h].start()

    x_far(1)
    x_near(1)
    routing = [
        rcopy(rwall.at[0], rwall.at[i], rw_ss.at[i], rw_rs.at[i], zdev(turn * ((i + 1) // 2) * (1 if i % 2 else -1)))
        for i in range(1, 8)
    ]
    for r in routing:
        r.start()
    for e in edges:
        e.wait_recv()
    prior = edge[0].astype(F32) * edge[1].astype(F32)
    prodp[0:16, :] = jnp.where(sp > 0, prior, jnp.zeros_like(prior))
    mix(0, 16)
    for n in range(4):
        got = jnp.dot(mixed[0:16, :], wproj_ref[:, n * COLS : (n + 1) * COLS], preferred_element_type=F32)
        pj[0, n // 2, 0:16, (n % 2) * COLS : (n % 2 + 1) * COLS] = got
    x_far(0)
    x_second(1)
    x_near(0)

    for r in routing:
        r.wait_recv()

    def tables(i, carry):
        rw = rwall[i]
        row = lax.broadcasted_iota(jnp.int32, (ROWS, ROWS), 0)
        lane = lax.broadcasted_iota(jnp.int32, (ROWS, ROWS), 1)
        expert = (z * 8 + row // CAP).astype(F32)
        slot = lax.rem(row, CAP).astype(F32)
        named = jnp.zeros((ROWS, ROWS), F32)
        weight = jnp.zeros((ROWS, ROWS), F32)
        for j in range(4):
            hit = rw[j : j + 1, :] == expert
            named = named + jnp.where(hit, 1.0, 0.0)
            weight = weight + jnp.where(hit, jnp.broadcast_to(rw[4 + j : 5 + j, :], (ROWS, ROWS)), 0.0)
        before = jnp.where(row < lane, 1.0, 0.0).astype(BF16)
        earlier = jnp.dot(named.astype(BF16), before, preferred_element_type=F32)
        picked = jnp.where(earlier == slot, named, 0.0)
        pmat[i] = picked.astype(BF16)
        wt = jnp.transpose(picked * weight)
        high = wt.astype(BF16)
        wmat[i, :, 0:ROWS] = high
        wmat[i, :, ROWS : 2 * ROWS] = (wt - high.astype(F32)).astype(BF16)
        return carry

    lax.fori_loop(0, 8, tables, 0)
    x_second(0)

    def ag(step, half, f):
        src = 0 if step == 0 else 2 * step - 1 if f else 2 * step
        dst = min(2 * step + 1 if f else 2 * step + 2, 7)
        at = (0 if f else 8) + 2 * step + half
        rows = halves[half]
        return rcopy(xs.at[src, rows], xs.at[dst, rows], ag_ss.at[at], ag_rs.at[at], zdev(turn if f else -turn))

    ring = {(s, h, f): ag(s, h, f) for s in range(3) for h in range(2) for f in (True, False)}
    ring[(3, 1, True)] = ag(3, 1, True)
    ring[(3, 0, False)] = ag(3, 0, False)

    def forward(step, half, f):
        ring[(step - 1, half, f)].wait_recv()
        if (step, half, f) in ring:
            ring[(step, half, f)].start()

    wide = (slice(0, 1024), slice(1024, 2048))

    def norms(at):
        proj = [pj[tp, n, at, :] + fm[n, at, :].astype(F32) + fp[n, at, :].astype(F32) for n in range(2)]
        square = sum(jnp.sum(p * p, axis=-1, keepdims=True) for p in proj)
        inv = lax.rsqrt(square * (1.0 / D) + EPS)
        st = [
            (resid_ref[at, wide[n]].astype(F32) + proj[n] * inv * post_ref[:, wide[n]]).astype(BF16)
            for n in range(2)
        ]
        square = jnp.zeros_like(square)
        for n in range(2):
            stream[at, wide[n]] = st[n]
            st[n] = st[n].astype(F32)
            square = square + jnp.sum(st[n] * st[n], axis=-1, keepdims=True)
        inv2 = lax.rsqrt(square * (1.0 / D) + EPS)
        for n in range(2):
            xs[0, at, wide[n]] = (st[n] * inv2 * pre_ref[:, wide[n]]).astype(BF16)

    def normed_rows(h):
        for name in ("one_b", "three_a", "one_a", "three_b"):
            x_sends[name, h].wait_recv()

        def half_rows(i, carry):
            norms(pl.ds(pl.multiple_of(h * HALF + i * 16, 16), 16))
            return carry

        lax.fori_loop(0, HALF // 16, half_rows, 0)

    def select(i):
        def cols(at):
            got = jnp.dot(pmat[i], xs[i, :, at], preferred_element_type=F32)
            sel[i, :, :, at] = got.astype(BF16).reshape(8, CAP, COLS)

        rows_loop(D // COLS, COLS, cols)

    sent, arriving, returned, coming = {}, {}, {}, {}
    for slot in range(8):
        for m, (dy, dc) in enumerate(MOVES):
            to, frm = in_plane(dy, dc), in_plane(-dy, dc)
            sems = d_ss.at[slot, m], d_rs.at[slot, m]
            sent[slot, m] = rcopy(sel.at[slot, to], rin.at[slot, k], *sems, pdev(to))
            arriving[slot, m] = rcopy(sel.at[slot, frm], rin.at[slot, frm], *sems, pdev(to))
            for ch in (0, 1) if slot in PARTED else (0,):
                cols = pl.ds(1024 * ch, 1024 if slot in PARTED else D)
                sems = r_ss.at[slot + 8 * ch, m], r_rs.at[slot + 8 * ch, m]
                returned[slot, ch, m] = rcopy(eout.at[slot, to, :, cols], rback.at[slot, k, :, cols], *sems, pdev(to))
                coming[slot, ch, m] = rcopy(eout.at[slot, frm, :, cols], rback.at[slot, frm, :, cols], *sems, pdev(to))

    def dispatch(slot):
        for m in range(7):
            sent[slot, m].start()
        rin[slot, k] = sel[slot, k]

    def send_back(slot, ch=0):
        for m in range(7):
            returned[slot, ch, m].start()

    def order_of(slot):
        return (1, 0) if slot % 2 == 1 else (0, 1)

    def experts(first, n, parted=False):
        for i in range(first, first + n):
            for m in range(7):
                arriving[i, m].wait_recv()
        if first == 0:
            for w in weights:
                w.wait()
        m = n * ROWS

        def gate_up(j, carry):
            x = rin[pl.ds(first, n)].reshape(m, D)
            gu = jnp.dot(x, wgu[j], preferred_element_type=F32)
            gate = jnp.minimum(gu[:, 0:128], 7.0)
            up = jnp.clip(gu[:, 128:256], -7.0, 7.0)
            hid[j, 0:m, :] = (gate * jax.nn.sigmoid(1.702 * gate) * (up + 1.0)).astype(BF16)
            return carry

        lax.fori_loop(0, 5, gate_up, 0)

        def down(at):
            h = jnp.concatenate([hid[j, 0:m, :] for j in range(5)], axis=1)
            got = jnp.dot(h, dwv[:, at], preferred_element_type=F32)
            eout[pl.ds(first, n), :, :, at] = got.astype(BF16).reshape(n, 8, CAP, COLS)

        if parted:
            for half in range(2):
                for n_ in range(2):
                    down(pl.ds(half * 1024 + n_ * COLS, COLS))
                send_back(7, half)
        else:
            rows_loop(D // COLS, COLS, down)
        for i in range(first, first + n):
            rback[i, k] = eout[i, k]

    normed_rows(1)
    ring[(0, 1, True)].start()
    ring[(0, 1, False)].start()
    normed_rows(0)
    ring[(0, 0, True)].start()
    ring[(0, 0, False)].start()
    select(0)
    dispatch(0)
    forward(1, 1, True)
    forward(1, 1, False)
    forward(1, 0, True)
    select(1)
    dispatch(1)
    forward(1, 0, False)
    select(2)
    dispatch(2)
    experts(0, 1)
    forward(2, 1, True)
    forward(2, 0, True)
    select(3)
    dispatch(3)
    forward(2, 1, False)
    forward(2, 0, False)
    select(4)
    dispatch(4)
    experts(1, 2)
    forward(3, 1, True)
    forward(3, 0, True)
    select(5)
    dispatch(5)
    forward(3, 0, False)
    forward(3, 1, False)
    select(6)
    ring[(3, 1, True)].wait_recv()
    ring[(3, 0, False)].wait_recv()
    select(7)
    dispatch(7)
    dispatch(6)
    experts(3, 2)
    experts(5, 1)
    experts(7, 1, True)
    for ch in order_of(5) if 5 in PARTED else (0,):
        send_back(5, ch)
    experts(6, 1)
    for slot in (6, 3, 4, 1, 2, 0):
        for ch in order_of(slot) if slot in PARTED else (0,):
            send_back(slot, ch)

    def combine(i, ch, dst, more=None):
        for n in range(2):
            at = slice(ch * 1024 + n * COLS, ch * 1024 + (n + 1) * COLS)
            here = slice(n * COLS, (n + 1) * COLS)
            r = rback[i, :, :, at].reshape(ROWS, COLS)
            got = jnp.dot(wmat[i, :, 0:ROWS], r, preferred_element_type=F32)
            got = got + jnp.dot(wmat[i, :, ROWS : 2 * ROWS], r, preferred_element_type=F32)
            if more is not None:
                got = got + more[:, here].astype(F32)
            dst[:, here] = got.astype(dst.dtype)

    def zsend(r, ch, f):
        at = (0 if f else 8) + 2 * r + ch
        src, dst = (sf, rf) if f else (ss, rs)
        return rcopy(src.at[r, ch], dst.at[r, ch], z_ss.at[at], z_rs.at[at], zdev(-turn if f else turn))

    chain = {(r, ch, f): zsend(r, ch, f) for r in range(1, 4) for ch in range(2) for f in (True, False)}
    chain[(0, 0, True)] = zsend(0, 0, True)
    chain[(0, 1, False)] = zsend(0, 1, False)

    def take(slot, ch=0):
        for m in range(7):
            coming[slot, ch, m].wait_recv()

    take(7)
    combine(7, 0, sf.at[0, 0])
    chain[(0, 0, True)].start()
    take(7, 1)
    combine(7, 1, ss.at[0, 1])
    chain[(0, 1, False)].start()
    for slot in (5, 6, 3, 4, 1, 2):
        f = slot % 2 == 1
        r = 4 - (slot + 1) // 2
        send, got = (sf, rf) if f else (ss, rs)
        if slot not in PARTED:
            take(slot)
        for ch in order_of(slot):
            if slot in PARTED:
                take(slot, ch)
            if (r - 1, ch, f) in chain:
                chain[(r - 1, ch, f)].wait_recv()
                combine(slot, ch, send.at[r, ch], got.at[r - 1, ch])
            else:
                combine(slot, ch, send.at[r, ch])
            chain[(r, ch, f)].start()

    take(0)
    combine(0, 0, part.at[0])
    combine(0, 1, part.at[1])
    for f, ch in ((True, 1), (True, 0), (False, 0), (False, 1)):
        chain[(3, ch, f)].wait_recv()

    def finish(at):
        total = [part[n, at, :] + rf[3, n, at, :].astype(F32) + rs[3, n, at, :].astype(F32) for n in range(2)]
        square = sum(jnp.sum(t * t, axis=-1, keepdims=True) for t in total)
        inv = lax.rsqrt(square * (1.0 / D) + EPS)
        for n in range(2):
            gained = total[n] * inv * moe_ref[:, wide[n]]
            out_ref[at, wide[n]] = (stream[at, wide[n]].astype(F32) + gained).astype(BF16)

    rows_loop(ROWS // 16, 16, finish)

    late = [ring[key] for key in ring]
    for group in (edges, routing, x_sends.values(), late, chain.values(), sent.values(), returned.values()):
        for s in group:
            s.wait_send()


def body(
    b_gate, c_gate, values_in, conv_taps, out_proj, resid, post_gain, pre_gain, moe_gain,
    routes, route_weight, gate_w, up_w, down_w,
):
    vmem = pl.BlockSpec(memory_space=pltpu.VMEM)
    hbm = pl.BlockSpec(memory_space=pl.ANY)
    dma = pltpu.SemaphoreType.DMA
    block = (ROWS, D)
    split = (2, ROWS, D // 2)
    return pl.pallas_call(
        kernel,
        out_shape=jax.ShapeDtypeStruct(block, BF16),
        in_specs=[hbm] * 5 + [vmem] * 6 + [hbm] * 3,
        out_specs=vmem,
        scratch_shapes=[
            pltpu.VMEM((512, 512), BF16),
            pltpu.VMEM((512, 512), BF16),
            pltpu.VMEM((512, 512), BF16),
            pltpu.VMEM((512, D), BF16),
            pltpu.VMEM(block, BF16),
            pltpu.VMEM((5, D, 256), BF16),
            pltpu.VMEM((FF, D), BF16),
            pltpu.VMEM((2, 16, 512), BF16),
            pltpu.VMEM((528, 512), F32),
            pltpu.VMEM((512, 512), BF16),
            pltpu.VMEM((4,) + split, F32),
            pltpu.VMEM(split, BF16),
            pltpu.VMEM(split, BF16),
            pltpu.VMEM(split, BF16),
            pltpu.VMEM((ROWS, D // 2), BF16),
            pltpu.VMEM((ROWS, D // 2), BF16),
            pltpu.VMEM(split, BF16),
            pltpu.VMEM(split, BF16),
            pltpu.VMEM(block, BF16),
            pltpu.VMEM((8,) + block, BF16),
            pltpu.VMEM((8, 8, 128), F32),
            pltpu.VMEM((8, ROWS, ROWS), BF16),
            pltpu.VMEM((8, ROWS, 2 * ROWS), BF16),
            pltpu.VMEM((8, 8, CAP, D), BF16),
            pltpu.VMEM((8, 8, CAP, D), BF16),
            pltpu.VMEM((5, 2 * ROWS, 128), BF16),
            pltpu.VMEM((8, 8, CAP, D), BF16),
            pltpu.VMEM((8, 8, CAP, D), BF16),
            pltpu.VMEM(split, F32),
            pltpu.VMEM((4,) + split, BF16),
            pltpu.VMEM((4,) + split, BF16),
            pltpu.VMEM((4,) + split, BF16),
            pltpu.VMEM((4,) + split, BF16),
            dma((5,)), dma((11,)),
            dma((2,)), dma((2,)),
            dma((8,)), dma((8,)),
            dma((12,)), dma((12,)),
            dma((16,)), dma((16,)),
            dma((8, 7)), dma((8, 7)),
            dma((16, 7)), dma((16, 7)),
            dma((16,)), dma((16,)),
        ],
        compiler_params=pltpu.CompilerParams(
            collective_id=0, has_side_effects=True, vmem_limit_bytes=63 * 2**20
        ),
    )(
        b_gate, c_gate, values_in, out_proj, resid, conv_taps,
        post_gain.reshape(1, D), pre_gain.reshape(1, D), moe_gain.reshape(1, D), routes.T, route_weight.T,
        gate_w, up_w, down_w,
    )


def solution(mesh):
    rows = P(("sp", "tp"), None)
    placed = (
        P("sp", "tp"), P("sp", "tp"), P("sp", "tp"), P(None, "tp"), P("tp", None), rows,
        P(), P(), P(), rows, rows,
        P("sp", None, None), P("sp", None, None), P("sp", None, None),
    )
    return jax.shard_map(body, mesh=mesh, in_specs=placed, out_specs=rows, check_vma=False)
```
